32 devices in a mesh: sp: 8 (over z, y), tp: 4 (over x, core).
Axes of the slice: x: 2, y: 2, z: 4, core: 2. Of those that a mesh axis runs over, the one named last changes fastest.
Arguments:
- stream: bfloat16 [2048, 2048], P('sp', 'tp'), may hold values from -8 to 8
- norm_gain: float32 [2, 2048], P(None, 'tp'), may hold values from 0.1 to 1.9
- query_weight: bfloat16 [2, 2048, 1024], P(None, None, 'tp'), may hold values from -4 to 4
- key_weight: bfloat16 [2, 2048, 1024], P(None, None, 'tp'), may hold values from -4 to 4
- value_weight: bfloat16 [2, 2048, 1024], P(None, None, 'tp'), may hold values from -0.125 to 0.125
- out_weight: bfloat16 [2, 1024, 2048], P(None, None, 'tp'), may hold values from -1.5 to 1.5
- rel_bias: float32 [2, 16, 257], P(None, 'tp'), may hold values from -4 to 4
Outputs:
- mixed: bfloat16 [2048, 2048], P('sp', 'tp')
The draws below stay inside these ranges and needn't reach their ends.
All inputs are finite; a program needn't handle non-finite values.
Results may differ from the reference program's by a relative error of at most 0.013.
Values may be sent and summed in bfloat16 or wider, within the bound.
A program may use at most 64 MiB of HBM per device.

```python
import math
import jax
import jax.numpy as jnp
from jax import lax

D = 2048
HEADS = 16
HEAD_DIM = 64
SEG = 64
PREV = 8
CLIP = 128
LAYERS = 2
TOKENS = 2048


def paired_weights(key):
    base_key = jax.random.fold_in(key, 7001)
    shape = (LAYERS, D, HEADS * HEAD_DIM)
    query_part = jax.random.normal(jax.random.fold_in(base_key, 1), shape, jnp.float32) * D ** (-0.5)
    other_part = jax.random.normal(jax.random.fold_in(base_key, 2), shape, jnp.float32) * D ** (-0.5)
    key_part = other_part
    return (jnp.clip(query_part, -4.0, 4.0), jnp.clip(key_part, -4.0, 4.0))


def draw_query_weight(key, part):
    return paired_weights(key)[0].astype(jnp.bfloat16)


def draw_key_weight(key, part):
    return paired_weights(key)[1].astype(jnp.bfloat16)


def draw_stream(key, part):
    ramp = jnp.exp(jnp.linspace(math.log(0.5), math.log(2.0), D, dtype=jnp.float32))
    jitter = jnp.exp(jax.random.uniform(jax.random.fold_in(key, 5005), (D,), jnp.float32, -0.35, 0.35))
    column_scale = (ramp * jitter)[None, :]
    base_rows = jnp.clip(jax.random.normal(jax.random.fold_in(key, 5001), (TOKENS, D), jnp.float32), -6.0, 6.0)
    return jnp.clip(base_rows * column_scale, -8.0, 8.0).astype(jnp.bfloat16)


def level_of(rng, dims, cuts, least, largest):
    def one(position, parts):
        steps = jax.random.uniform(jax.random.fold_in(jax.random.fold_in(rng, 6), position), (parts,), jnp.float32, least / len(cuts), largest / len(cuts))
        return jnp.repeat(jnp.exp(steps), dims[position] // parts).reshape((-1,) + (1,) * (len(dims) - position - 1))

    factor_of = one(*cuts[0])
    for cut in cuts[1:]:
        factor_of = factor_of * one(*cut)
    return factor_of


def scatter_about(key, extent, spread, limit, shards=(), kind=jnp.bfloat16):
    result = spread * jax.random.normal(key, extent, jnp.float32)
    if shards:
        result = result * level_of(key, extent, shards, -0.22, 0.18)
    return jnp.clip(result, -limit, limit).astype(kind)


def setup_inputs(seed: int = 0) -> dict:
    keys = jax.random.split(jax.random.key(seed), 8)
    stream = draw_stream(jax.random.fold_in(keys[7], 71), 0)
    norm_gain = jnp.clip(1.0 + 0.18 * jax.random.normal(keys[1], (LAYERS, D), jnp.float32), 0.1, 1.9)
    query_weight = draw_query_weight(jax.random.fold_in(keys[7], 71), 0)
    key_weight = draw_key_weight(jax.random.fold_in(keys[7], 71), 0)
    value_weight = scatter_about(keys[4], (LAYERS, D, HEADS * HEAD_DIM), D ** -0.5, 0.125, ((2, 4),))
    out_weight = scatter_about(keys[5], (LAYERS, HEADS * HEAD_DIM, D), (HEADS * HEAD_DIM // 64) ** -0.5, 1.5, ((2, 4),))
    rel_bias = scatter_about(keys[6], (LAYERS, HEADS, 2 * CLIP + 1), 1.0, 4.0, ((1, 4),), jnp.float32)
    return dict(stream=stream, norm_gain=norm_gain, query_weight=query_weight, key_weight=key_weight, value_weight=value_weight, out_weight=out_weight, rel_bias=rel_bias)


epsilon = 1e-06
masked_score = -1e+30

def normalize(residual, gain):
    values_f = residual.astype(jnp.float32)
    scaled = values_f * lax.rsqrt(lax.optimization_barrier(jnp.mean(values_f * values_f, axis=-1, keepdims=True)) + epsilon)
    return (scaled * gain).astype(jnp.bfloat16)

def distance_index(band_len):
    within = jnp.arange(SEG, dtype=jnp.int32)[:, None]
    across = jnp.arange(band_len, dtype=jnp.int32)[None, :]
    return jnp.minimum(band_len - SEG + within - across, CLIP) + CLIP

def reference(stream, norm_gain, query_weight, key_weight, value_weight, out_weight, rel_bias):
    reach_rows = PREV * SEG
    band_len = reach_rows + SEG
    head_cols = HEADS * HEAD_DIM
    table_index = distance_index(band_len)
    residual = stream
    for layer_index in range(LAYERS):
        normed = normalize(residual, norm_gain[layer_index])
        query_rows = jnp.dot(normed, query_weight[layer_index], preferred_element_type=jnp.float32).astype(jnp.bfloat16)
        key_rows = jnp.dot(normed, key_weight[layer_index], preferred_element_type=jnp.float32).astype(jnp.bfloat16)
        value_rows = jnp.dot(normed, value_weight[layer_index], preferred_element_type=jnp.float32).astype(jnp.bfloat16)
        padding = jnp.zeros((reach_rows, head_cols), jnp.bfloat16)
        key_ext = jnp.concatenate([padding, key_rows], axis=0)
        value_ext = jnp.concatenate([padding, value_rows], axis=0)
        position_bias = rel_bias[layer_index][:, table_index]

        def one_segment(segment):
            start = (segment * SEG).astype(jnp.int32)
            queries = lax.dynamic_slice_in_dim(query_rows, start, SEG, 0).astype(jnp.float32).reshape(SEG, HEADS, HEAD_DIM)
            keys_band = lax.dynamic_slice_in_dim(key_ext, start, band_len, 0).astype(jnp.float32).reshape(band_len, HEADS, HEAD_DIM)
            values_band = lax.dynamic_slice_in_dim(value_ext, start, band_len, 0).astype(jnp.float32).reshape(band_len, HEADS, HEAD_DIM)
            visible = start - reach_rows + jnp.arange(band_len, dtype=jnp.int32) >= 0
            scores = jnp.einsum('qhd,khd->hqk', queries, keys_band) * HEAD_DIM ** (-0.5) + position_bias
            scores = jnp.where(visible[None, None, :], scores, masked_score)
            maximum = lax.optimization_barrier(jnp.max(scores, axis=-1, keepdims=True))
            exponent = jnp.exp(scores - maximum)
            weights = (exponent / lax.optimization_barrier(jnp.sum(exponent, axis=-1, keepdims=True))).astype(jnp.bfloat16)
            attended = jnp.einsum('hqk,khd->qhd', weights.astype(jnp.float32), values_band)
            return attended.astype(jnp.bfloat16).reshape(SEG, head_cols)
        attended = lax.map(one_segment, jnp.arange(TOKENS // SEG, dtype=jnp.int32)).reshape(TOKENS, head_cols)
        total = jnp.dot(attended, out_weight[layer_index], preferred_element_type=jnp.float32)
        residual = (residual.astype(jnp.float32) + total).astype(jnp.bfloat16)
    return residual
```

```python
import functools

import jax
import jax.numpy as jnp
from jax import lax
from jax.experimental import pallas as pl
from jax.experimental.pallas import tpu as pltpu
from jax.sharding import PartitionSpec as P

SEG = 64
PREV = 8
CLIP = 128
LANES = 128
CHUNKS = 4
PAIR = 2 * SEG
REACH = PREV * SEG
BAND = REACH + PAIR

epsilon = 1e-06
masked_score = -1e30
MESH = pl.DeviceIdType.MESH


class Gather:
    def __init__(self, n_tp, slot, send_sems, recv_sems):
        self.n_x = n_tp // 2
        self.me = lax.axis_index("tp")
        self.core = lax.rem(self.me, 2)
        self.x = self.me // 2
        self.sibling = self.me + 1 - 2 * self.core
        self.slot, self.send_sems, self.recv_sems = slot, send_sems, recv_sems

    def across(self, step, core):
        return lax.rem(self.x + step, self.n_x) * 2 + core

    def copy(self, source, origin, part, index, target):
        return pltpu.make_async_remote_copy(
            src_ref=source,
            dst_ref=self.slot(origin, part),
            send_sem=self.send_sems.at[part, index],
            recv_sem=self.recv_sems.at[part, origin],
            device_id={"tp": target},
            device_id_type=MESH,
        )

    def own(self, part, source=None):
        source = self.slot(self.me, part) if source is None else source
        targets = [self.across(s, self.core) for s in range(1, self.n_x)] + [self.sibling]
        return [self.copy(source, self.me, part, i, t) for i, t in enumerate(targets)]

    def send(self, part, source=None):
        for copy in self.own(part, source):
            copy.start()

    def relays(self, part):
        out = []
        for s in range(1, self.n_x):
            origin = self.across(s, self.core)
            out.append(
                self.copy(self.slot(origin, part), origin, part, self.n_x - 1 + s, self.sibling)
            )
        return out

    def relay(self, part):
        for copy in self.relays(part):
            copy.wait_recv()
            copy.start()

    def others(self):
        return [self.sibling] + [self.across(s, 1 - self.core) for s in range(1, self.n_x)]

    def wait_slot(self, part, origin):
        self.copy(self.slot(origin, part), origin, part, 0, self.sibling).wait_recv()

    def wait_rest(self, part):
        for origin in self.others():
            self.wait_slot(part, origin)

    def finish(self, part, source=None):
        for copy in self.own(part, source) + self.relays(part):
            copy.wait_send()


def kernel(
    n_tp, n_sp, head_dim,
    stream, gain, query_w, key_w, value_w, out_w, base,
    out,
    xg, gg, wq, wk, wv, wo, normed, bias, qx, kx, vx, att,
    xs, xr, ats, atr, kvs, kvr, gs, gr, wsem, own_sem,
):
    layers, _, rows, width = xg.shape
    groups = kx.shape[1]
    head_cols = groups * LANES
    per_group = LANES // head_dim
    total_width = n_tp * width
    shift = REACH // rows
    sp = lax.axis_index("sp")
    tp = lax.axis_index("tp")
    relayed = shift == 2 and n_sp % 2 == 0

    weights = []
    for l in range(layers):
        pairs = ((key_w, wk), (value_w, wv), (query_w, wq), (out_w, wo))
        weights.append(
            [pltpu.make_async_copy(s.at[l], d.at[l], wsem.at[l, i]) for i, (s, d) in enumerate(pairs)]
        )
    own_stream = pltpu.make_async_copy(stream, xg.at[0, tp], own_sem.at[0])
    own_gain = pltpu.make_async_copy(gain, gg.at[tp], own_sem.at[1])
    own_stream.start()
    own_gain.start()

    barrier = pltpu.get_barrier_semaphore()
    for d in range(1, n_tp):
        pl.semaphore_signal(
            barrier, inc=1, device_id={"tp": lax.rem(tp + d, n_tp)}, device_id_type=MESH
        )
    count = n_tp - 1
    for d in range(1, shift + 1):

        @pl.when(sp + d < n_sp)
        def _():
            pl.semaphore_signal(barrier, inc=1, device_id={"sp": sp + d}, device_id_type=MESH)

        @pl.when(sp >= d)
        def _():
            pl.semaphore_signal(barrier, inc=1, device_id={"sp": sp - d}, device_id_type=MESH)

        count = count + jnp.where(sp + d < n_sp, 1, 0) + jnp.where(sp >= d, 1, 0)
    for copy in weights[0]:
        copy.start()
    pl.semaphore_wait(barrier, count)

    piece = rows // CHUNKS
    xgather = [
        Gather(
            n_tp,
            lambda j, c, l=l: xg.at[l, j, pl.ds(c * piece, piece)],
            xs.at[l],
            xr.at[l],
        )
        for l in range(layers)
    ]
    agather = [
        Gather(n_tp, lambda j, g, l=l: att.at[l, j, g], ats.at[l], atr.at[l])
        for l in range(layers)
    ]

    def stream_piece(c):
        return stream.at[pl.ds(c * piece, piece)]

    for c in range(CHUNKS):
        xgather[0].send(c, stream_piece(c))
    gain_copies = [
        pltpu.make_async_remote_copy(
            src_ref=gain,
            dst_ref=gg.at[tp],
            send_sem=gs.at[d - 1],
            recv_sem=gr.at[d - 1],
            device_id={"tp": lax.rem(tp + d, n_tp)},
            device_id_type=MESH,
        )
        for d in range(1, n_tp)
    ]
    for copy in gain_copies:
        copy.start()
    for l in range(1, layers):
        for copy in weights[l]:
            copy.start()

    for l in range(layers):
        for d in range(1, shift + 1):

            @pl.when(sp < d)
            def _():
                empty = jnp.zeros((rows, LANES), jnp.bfloat16)
                for g in range(groups):
                    kx[l, g, pl.ds((shift - d) * rows, rows), :] = empty
                    vx[l, g, pl.ds((shift - d) * rows, rows), :] = empty

    wide = base.shape[-1]
    seg_q = lax.broadcasted_iota(jnp.int32, (PAIR, BAND), 0) // SEG
    seg_k = lax.broadcasted_iota(jnp.int32, (PAIR, BAND), 1) // SEG
    seen = (seg_k >= seg_q) & (seg_k <= seg_q + PREV)
    for l in range(layers):
        for g in range(groups):
            for h in range(per_group):
                row = base[l, g * per_group + h : g * per_group + h + 1, :]
                table = pltpu.roll(
                    jnp.broadcast_to(row, (PAIR, wide)), 0, 1, stride=1, stride_axis=0
                )[:, :BAND]
                bias[l, g, h * PAIR : (h + 1) * PAIR, :] = jnp.where(seen, table, masked_score)

    tensors = (kx, vx)

    def halo_copy(l, t, g, from_slot, to_slot, index, target):
        buf = tensors[t]
        return pltpu.make_async_remote_copy(
            src_ref=buf.at[l, g, pl.ds(from_slot * rows, rows)],
            dst_ref=buf.at[l, g, pl.ds(to_slot * rows, rows)],
            send_sem=kvs.at[l, t, g, index],
            recv_sem=kvr.at[l, t, g, to_slot],
            device_id={"sp": target},
            device_id_type=MESH,
        )

    even = lax.rem(sp, 2) == 0
    odd_behind = (lax.rem(sp, 2) == 1) & (sp >= 2)

    def direct_copies(l, t, g):
        out_list = []
        for d in range(shift, 0, -1):
            ok = sp + d < n_sp
            if relayed and d == 1:
                ok = even
            out_list.append((ok, halo_copy(l, t, g, shift, shift - d, d - 1, sp + d)))
        return out_list

    def relay_copy(l, t, g):
        return halo_copy(l, t, g, 0, 1, shift, sp - 1)

    def halo_send(l, t, g):
        for ok, copy in direct_copies(l, t, g):
            pl.when(ok)(copy.start)

    def halo_wait(l, t, g):
        for d in range(shift, 0, -1):
            slot = shift - d

            @pl.when(sp >= d)
            def _():
                halo_copy(l, t, g, slot, slot, 0, lax.rem(sp + 1, n_sp)).wait_recv()

            if relayed and d == 2:
                pl.when(odd_behind)(relay_copy(l, t, g).start)

    own_gain.wait()
    for d in range(1, n_tp):
        pltpu.make_async_remote_copy(
            src_ref=gain,
            dst_ref=gg.at[lax.rem(tp - d + n_tp, n_tp)],
            send_sem=gs.at[d - 1],
            recv_sem=gr.at[d - 1],
            device_id={"tp": lax.rem(tp + d, n_tp)},
            device_id_type=MESH,
        ).wait_recv()
    own_stream.wait()

    lane = lax.broadcasted_iota(jnp.int32, (PAIR, LANES), 1) // head_dim
    scale = head_dim ** (-0.5)

    for l in range(layers):
        gather = xgather[l]
        for c in range(CHUNKS):
            gather.relay(c)
        for c in range(CHUNKS):
            gather.wait_rest(c)
            span = slice(c * piece, (c + 1) * piece)
            squares = jnp.zeros((piece, 1), jnp.float32)
            for j in range(n_tp):
                part = xg[l, j, span, :].astype(jnp.float32)
                squares = squares + jnp.sum(part * part, axis=-1, keepdims=True)
            inverse = lax.rsqrt(squares / total_width + epsilon)
            for j in range(n_tp):
                part = xg[l, j, span, :].astype(jnp.float32) * inverse
                normed[span, j * width : (j + 1) * width] = (
                    part * gg[j, l : l + 1, :]
                ).astype(jnp.bfloat16)

        for t, (buf, mat) in enumerate(((kx, wk), (vx, wv))):
            weights[l][t].wait()
            made = jnp.dot(normed[...], mat[l], preferred_element_type=jnp.float32)
            made = made.astype(jnp.bfloat16)
            for g in range(groups):
                buf[l, g, shift * rows :, :] = made[:, g * LANES : (g + 1) * LANES]
            if t == 0:
                halo_send(l, 0, 0)
        halo_send(l, 1, 0)
        for g in range(1, groups):
            halo_send(l, 0, g)
            halo_send(l, 1, g)
        weights[l][2].wait()
        qx[...] = (
            jnp.dot(normed[...], wq[l], preferred_element_type=jnp.float32) * scale
        ).astype(jnp.bfloat16)

        for g in range(groups):
            for t in range(2):
                halo_wait(l, t, g)
            for b in range(rows // PAIR):
                block = qx[b * PAIR : (b + 1) * PAIR, g * LANES : (g + 1) * LANES]
                stacked = jnp.concatenate(
                    [jnp.where(lane == h, block, jnp.zeros_like(block)) for h in range(per_group)],
                    axis=0,
                )
                keys = kx[l, g, b * PAIR : b * PAIR + BAND, :]
                values = vx[l, g, b * PAIR : b * PAIR + BAND, :]
                position = (
                    sp * rows - REACH + b * PAIR
                    + lax.broadcasted_iota(jnp.int32, (1, BAND), 1)
                )
                hidden = jnp.where(position >= 0, 0.0, masked_score)
                scores = lax.dot_general(
                    stacked, keys, (((1,), (1,)), ((), ())), preferred_element_type=jnp.float32
                )
                scores = scores + bias[l, g] + hidden
                top = jnp.max(scores, axis=-1, keepdims=True)
                grown = jnp.exp(scores - top)
                summed = jnp.sum(grown, axis=-1, keepdims=True)
                mix = jnp.dot(
                    grown.astype(jnp.bfloat16), values, preferred_element_type=jnp.float32
                )
                mix = mix / summed
                chosen = mix[:PAIR]
                for h in range(1, per_group):
                    chosen = jnp.where(lane == h, mix[h * PAIR : (h + 1) * PAIR], chosen)
                att[l, tp, g, b * PAIR : (b + 1) * PAIR, :] = chosen.astype(jnp.bfloat16)
            agather[l].send(g)

        gather = agather[l]
        weights[l][3].wait()

        def mixed_part(j):
            wide_rows = jnp.concatenate([att[l, j, g] for g in range(groups)], axis=1)
            mat = wo[l, pl.ds(pl.multiple_of(j * head_cols, LANES), head_cols), :]
            return jnp.dot(wide_rows, mat, preferred_element_type=jnp.float32)

        total = xg[l, tp].astype(jnp.float32) + mixed_part(tp)
        for g in range(groups):
            gather.relay(g)
        for s in range(1, gather.n_x):
            total = total + mixed_part(gather.across(s, gather.core))
        for origin in gather.others():
            for g in range(groups):
                gather.wait_slot(g, origin)
            total = total + mixed_part(origin)
        result = total.astype(jnp.bfloat16)
        if l + 1 < layers:
            xg[l + 1, tp] = result
            for c in range(CHUNKS):
                xgather[l + 1].send(c)
        else:
            out[...] = result

    for copy in gain_copies:
        copy.wait_send()
    for l in range(layers):
        for c in range(CHUNKS):
            xgather[l].finish(c, stream_piece(c) if l == 0 else None)
        for g in range(groups):
            agather[l].finish(g)
            for t in range(2):
                for ok, copy in direct_copies(l, t, g):
                    pl.when(ok)(copy.wait_send)
                if relayed:
                    pl.when(odd_behind)(relay_copy(l, t, g).wait_send)


def per_device(n_tp, n_sp, stream, norm_gain, query_weight, key_weight, value_weight, out_weight, rel_bias):
    rows, width = stream.shape
    layers, full, head_cols = query_weight.shape
    heads_here = rel_bias.shape[1]
    head_dim = head_cols // heads_here
    groups = head_cols // LANES
    n_x = n_tp // 2
    shift = REACH // rows
    far = rel_bias[:, :, 2 * CLIP :]
    base = jnp.concatenate(
        [
            jnp.broadcast_to(far, (layers, heads_here, REACH - CLIP)),
            rel_bias[:, :, :0:-1],
            jnp.broadcast_to(far, (layers, heads_here, PAIR)),
        ],
        axis=2,
    )
    any_space = pl.BlockSpec(memory_space=pl.ANY)
    vmem = pl.BlockSpec(memory_space=pltpu.VMEM)
    bf16, f32 = jnp.bfloat16, jnp.float32
    dma = pltpu.SemaphoreType.DMA
    return pl.pallas_call(
        functools.partial(kernel, n_tp, n_sp, head_dim),
        out_shape=jax.ShapeDtypeStruct((rows, width), bf16),
        in_specs=[any_space] * 6 + [vmem],
        out_specs=vmem,
        scratch_shapes=[
            pltpu.VMEM((layers, n_tp, rows, width), bf16),
            pltpu.VMEM((n_tp, layers, width), f32),
            pltpu.VMEM((layers, full, head_cols), bf16),
            pltpu.VMEM((layers, full, head_cols), bf16),
            pltpu.VMEM((layers, full, head_cols), bf16),
            pltpu.VMEM((layers, n_tp * head_cols, width), bf16),
            pltpu.VMEM((rows, full), bf16),
            pltpu.VMEM((layers, groups, (LANES // head_dim) * PAIR, BAND), f32),
            pltpu.VMEM((rows, head_cols), bf16),
            pltpu.VMEM((layers, groups, REACH + rows, LANES), bf16),
            pltpu.VMEM((layers, groups, REACH + rows, LANES), bf16),
            pltpu.VMEM((layers, n_tp, groups, rows, LANES), bf16),
            dma((layers, CHUNKS, 2 * n_x - 1)),
            dma((layers, CHUNKS, n_tp)),
            dma((layers, groups, 2 * n_x - 1)),
            dma((layers, groups, n_tp)),
            dma((layers, 2, groups, shift + 1)),
            dma((layers, 2, groups, shift)),
            dma((n_tp - 1,)),
            dma((n_tp - 1,)),
            dma((layers, 4)),
            dma((2,)),
        ],
        compiler_params=pltpu.CompilerParams(
            collective_id=0, has_side_effects=True, vmem_limit_bytes=60 * 1024 * 1024
        ),
    )(stream, norm_gain, query_weight, key_weight, value_weight, out_weight, base)


def solution(mesh):
    placed = (
        P("sp", "tp"),
        P(None, "tp"),
        P(None, None, "tp"),
        P(None, None, "tp"),
        P(None, None, "tp"),
        P(None, None, "tp"),
        P(None, "tp", None),
    )
    return jax.shard_map(
        functools.partial(per_device, mesh.shape["tp"], mesh.shape["sp"]),
        mesh=mesh, in_specs=placed, out_specs=P("sp", "tp"), check_vma=False,
    )
```

```python
import functools

import jax
import jax.numpy as jnp
from jax import lax
from jax.experimental import pallas as pl
from jax.experimental.pallas import tpu as pltpu
from jax.sharding import PartitionSpec as P

SEG = 64
PREV = 8
CLIP = 128
LANES = 128
CHUNKS = 4
PAIR = 2 * SEG
REACH = PREV * SEG
BAND = REACH + PAIR

epsilon = 1e-06
masked_score = -1e30
MESH = pl.DeviceIdType.MESH


class Gather:
    def __init__(self, n_tp, slot, send_sems, recv_sems):
        self.n_x = n_tp // 2
        self.me = lax.axis_index("tp")
        self.core = lax.rem(self.me, 2)
        self.x = self.me // 2
        self.sibling = self.me + 1 - 2 * self.core
        self.slot, self.send_sems, self.recv_sems = slot, send_sems, recv_sems

    def across(self, step, core):
        return lax.rem(self.x + step, self.n_x) * 2 + core

    def copy(self, source, origin, part, index, target):
        return pltpu.make_async_remote_copy(
            src_ref=source,
            dst_ref=self.slot(origin, part),
            send_sem=self.send_sems.at[part, index],
            recv_sem=self.recv_sems.at[part, origin],
            device_id={"tp": target},
            device_id_type=MESH,
        )

    def own(self, part, source=None):
        source = self.slot(self.me, part) if source is None else source
        targets = [self.across(s, self.core) for s in range(1, self.n_x)] + [self.sibling]
        return [self.copy(source, self.me, part, i, t) for i, t in enumerate(targets)]

    def send(self, part, source=None):
        for copy in self.own(part, source):
            copy.start()

    def relays(self, part):
        out = []
        for s in range(1, self.n_x):
            origin = self.across(s, self.core)
            out.append(
                self.copy(self.slot(origin, part), origin, part, self.n_x - 1 + s, self.sibling)
            )
        return out

    def relay(self, part):
        for copy in self.relays(part):
            copy.wait_recv()
            copy.start()

    def others(self):
        return [self.sibling] + [self.across(s, 1 - self.core) for s in range(1, self.n_x)]

    def wait_slot(self, part, origin):
        self.copy(self.slot(origin, part), origin, part, 0, self.sibling).wait_recv()

    def wait_rest(self, part):
        for origin in self.others():
            self.wait_slot(part, origin)

    def finish(self, part, source=None):
        for copy in self.own(part, source) + self.relays(part):
            copy.wait_send()


def kernel(
    n_tp, n_sp, head_dim,
    stream, gain, query_w, key_w, value_w, out_w, rel_bias,
    out,
    xg, gg, table, wq, wk, wv, wo, normed, bias, qx, kx, vx, att,
    xs, xr, ats, atr, kvs, kvr, gs, gr, wsem, own_sem,
):
    layers, _, rows, width = xg.shape
    groups = kx.shape[1]
    head_cols = groups * LANES
    per_group = LANES // head_dim
    total_width = n_tp * width
    shift = REACH // rows
    sp = lax.axis_index("sp")
    tp = lax.axis_index("tp")
    relayed = shift == 2 and n_sp % 2 == 0
    blocks = rows // PAIR
    per_block = CHUNKS // blocks

    weights = []
    for l in range(layers):
        pairs = ((key_w, wk), (value_w, wv), (query_w, wq), (out_w, wo))
        weights.append(
            [pltpu.make_async_copy(s.at[l], d.at[l], wsem.at[l, i]) for i, (s, d) in enumerate(pairs)]
        )
    own_stream = pltpu.make_async_copy(stream, xg.at[0, tp], own_sem.at[0])
    own_gain = pltpu.make_async_copy(gain, gg.at[tp], own_sem.at[1])
    own_stream.start()
    own_gain.start()
    own_table = pltpu.make_async_copy(rel_bias, table, own_sem.at[2])
    own_table.start()

    barrier = pltpu.get_barrier_semaphore()
    for d in range(1, n_tp):
        pl.semaphore_signal(
            barrier, inc=1, device_id={"tp": lax.rem(tp + d, n_tp)}, device_id_type=MESH
        )
    count = n_tp - 1
    for d in range(1, shift + 1):

        @pl.when(sp + d < n_sp)
        def _():
            pl.semaphore_signal(barrier, inc=1, device_id={"sp": sp + d}, device_id_type=MESH)

        @pl.when(sp >= d)
        def _():
            pl.semaphore_signal(barrier, inc=1, device_id={"sp": sp - d}, device_id_type=MESH)

        count = count + jnp.where(sp + d < n_sp, 1, 0) + jnp.where(sp >= d, 1, 0)
    for copy in weights[0]:
        copy.start()
    pl.semaphore_wait(barrier, count)

    piece = rows // CHUNKS
    xgather = [
        Gather(
            n_tp,
            lambda j, c, l=l: xg.at[l, j, pl.ds(c * piece, piece)],
            xs.at[l],
            xr.at[l],
        )
        for l in range(layers)
    ]
    agather = [
        Gather(n_tp, lambda j, b, l=l: att.at[l, j, b], ats.at[l], atr.at[l])
        for l in range(layers)
    ]

    def stream_piece(c):
        return stream.at[pl.ds(c * piece, piece)]

    for c in range(CHUNKS):
        xgather[0].send(c, stream_piece(c))
    gain_copies = [
        pltpu.make_async_remote_copy(
            src_ref=gain,
            dst_ref=gg.at[tp],
            send_sem=gs.at[d - 1],
            recv_sem=gr.at[d - 1],
            device_id={"tp": lax.rem(tp + d, n_tp)},
            device_id_type=MESH,
        )
        for d in range(1, n_tp)
    ]
    for copy in gain_copies:
        copy.start()
    for l in range(1, layers):
        for copy in weights[l]:
            copy.start()

    for l in range(layers):
        for d in range(1, shift + 1):

            @pl.when(sp < d)
            def _():
                empty = jnp.zeros((rows, LANES), jnp.bfloat16)
                for g in range(groups):
                    kx[l, g, pl.ds((shift - d) * rows, rows), :] = empty
                    vx[l, g, pl.ds((shift - d) * rows, rows), :] = empty

    own_table.wait()
    near = 2 * CLIP
    flip = (
        lax.broadcasted_iota(jnp.int32, (near, near), 0)
        + lax.broadcasted_iota(jnp.int32, (near, near), 1)
        == near - 1
    ).astype(jnp.float32)
    seg_q = lax.broadcasted_iota(jnp.int32, (PAIR, BAND), 0) // SEG
    seg_k = lax.broadcasted_iota(jnp.int32, (PAIR, BAND), 1) // SEG
    seen = (seg_k >= seg_q) & (seg_k <= seg_q + PREV)
    for l in range(layers):
        heads = table.shape[1]
        turned = jnp.dot(
            table[l][:, 1:], flip, precision=lax.Precision.HIGHEST,
            preferred_element_type=jnp.float32,
        )
        far = table[l][:, near:]
        base = jnp.concatenate(
            [
                jnp.broadcast_to(far, (heads, REACH - CLIP)),
                turned,
                jnp.broadcast_to(far, (heads, PAIR)),
            ],
            axis=1,
        )
        for h in range(heads):
            spread = jnp.broadcast_to(base[h : h + 1], (PAIR, base.shape[1]))
            shifted = pltpu.roll(spread, 0, 1, stride=1, stride_axis=0)[:, :BAND]
            first = h % per_group * PAIR
            bias[l, h // per_group, first : first + PAIR, :] = jnp.where(
                seen, shifted, masked_score
            )

    tensors = (kx, vx)

    def halo_copy(l, t, g, half, from_slot, to_slot, index, target):
        buf = tensors[t]
        return pltpu.make_async_remote_copy(
            src_ref=buf.at[l, g, pl.ds(from_slot * rows + half * PAIR, PAIR)],
            dst_ref=buf.at[l, g, pl.ds(to_slot * rows + half * PAIR, PAIR)],
            send_sem=kvs.at[l, t, g * blocks + half, index],
            recv_sem=kvr.at[l, t, g * blocks + half, to_slot],
            device_id={"sp": target},
            device_id_type=MESH,
        )

    even = lax.rem(sp, 2) == 0
    odd_behind = (lax.rem(sp, 2) == 1) & (sp >= 2)

    def direct_copies(l, t, g, half):
        out_list = []
        for d in range(shift, 0, -1):
            ok = sp + d < n_sp
            if relayed and d == 1:
                ok = even
            out_list.append((ok, halo_copy(l, t, g, half, shift, shift - d, d - 1, sp + d)))
        return out_list

    def relay_copy(l, t, g, half):
        return halo_copy(l, t, g, half, 0, 1, shift, sp - 1)

    def halo_send(l, half):
        for g in range(groups):
            for t in range(2):
                for ok, copy in direct_copies(l, t, g, half):
                    pl.when(ok)(copy.start)

    def halo_wait_slot(l, t, g, half, d):
        @pl.when(sp >= d)
        def _():
            slot = shift - d
            halo_copy(l, t, g, half, slot, slot, 0, lax.rem(sp + 1, n_sp)).wait_recv()

    def halo_far(l, g, half):
        for t in range(2):
            halo_wait_slot(l, t, g, half, shift)
            if relayed:
                pl.when(odd_behind)(relay_copy(l, t, g, half).start)

    def halo_near(l, g, half):
        for t in range(2):
            for d in range(shift - 1, 0, -1):
                halo_wait_slot(l, t, g, half, d)

    own_gain.wait()
    for d in range(1, n_tp):
        pltpu.make_async_remote_copy(
            src_ref=gain,
            dst_ref=gg.at[lax.rem(tp - d + n_tp, n_tp)],
            send_sem=gs.at[d - 1],
            recv_sem=gr.at[d - 1],
            device_id={"tp": lax.rem(tp + d, n_tp)},
            device_id_type=MESH,
        ).wait_recv()
    own_stream.wait()

    lane = lax.broadcasted_iota(jnp.int32, (PAIR, LANES), 1) // head_dim
    scale = head_dim ** (-0.5)

    def normalize(l, c):
        span = slice(c * piece, (c + 1) * piece)
        squares = jnp.zeros((piece, 1), jnp.float32)
        for j in range(n_tp):
            part = xg[l, j, span, :].astype(jnp.float32)
            squares = squares + jnp.sum(part * part, axis=-1, keepdims=True)
        inverse = lax.rsqrt(squares / total_width + epsilon)
        for j in range(n_tp):
            part = xg[l, j, span, :].astype(jnp.float32) * inverse
            normed[span, j * width : (j + 1) * width] = (
                part * gg[j, l : l + 1, :]
            ).astype(jnp.bfloat16)

    def block_rows(b):
        return slice(b * PAIR, (b + 1) * PAIR)

    def keys_values(l, b):
        for t, (buf, mat) in enumerate(((kx, wk), (vx, wv))):
            if b == 0:
                weights[l][t].wait()
            made = jnp.dot(normed[block_rows(b), :], mat[l], preferred_element_type=jnp.float32)
            made = made.astype(jnp.bfloat16)
            first = shift * rows + b * PAIR
            for g in range(groups):
                buf[l, g, first : first + PAIR, :] = made[:, g * LANES : (g + 1) * LANES]

    def attend(l, b, g):
        lanes = slice(g * LANES, (g + 1) * LANES)
        block = qx[block_rows(b), lanes]
        stacked = jnp.concatenate(
            [jnp.where(lane == h, block, jnp.zeros_like(block)) for h in range(per_group)], axis=0
        )
        keys = kx[l, g, b * PAIR : b * PAIR + BAND, :]
        values = vx[l, g, b * PAIR : b * PAIR + BAND, :]
        position = sp * rows - REACH + b * PAIR + lax.broadcasted_iota(jnp.int32, (1, BAND), 1)
        hidden = jnp.where(position >= 0, 0.0, masked_score)
        scores = lax.dot_general(
            stacked, keys, (((1,), (1,)), ((), ())), preferred_element_type=jnp.float32
        )
        scores = scores + bias[l, g] + hidden
        top = jnp.max(scores, axis=-1, keepdims=True)
        grown = jnp.exp(scores - top)
        summed = jnp.sum(grown, axis=-1, keepdims=True)
        mix = jnp.dot(grown.astype(jnp.bfloat16), values, preferred_element_type=jnp.float32)
        mix = mix / summed
        chosen = mix[:PAIR]
        for h in range(1, per_group):
            chosen = jnp.where(lane == h, mix[h * PAIR : (h + 1) * PAIR], chosen)
        att[l, tp, b, :, lanes] = chosen.astype(jnp.bfloat16)

    def mixed_part(l, b, j):
        mat = wo[l, pl.ds(pl.multiple_of(j * head_cols, LANES), head_cols), :]
        return jnp.dot(att[l, j, b], mat, preferred_element_type=jnp.float32)

    for l in range(layers):
        gather = xgather[l]
        gather.relay(0)
        for b in range(blocks):
            for c in range(b * per_block, (b + 1) * per_block):
                if c + 1 < CHUNKS:
                    gather.relay(c + 1)
                gather.wait_rest(c)
                normalize(l, c)
            keys_values(l, b)
            halo_send(l, b)
        weights[l][2].wait()
        for b in range(blocks):
            if b + 1 < blocks:
                for g in range(groups):
                    halo_far(l, g, b)
            qx[block_rows(b), :] = (
                jnp.dot(normed[block_rows(b), :], wq[l], preferred_element_type=jnp.float32) * scale
            ).astype(jnp.bfloat16)
        for g in range(groups):
            halo_far(l, g, blocks - 1)
        for b in range(blocks):
            for g in range(groups):
                if b == 0:
                    for half in range(blocks):
                        halo_near(l, g, half)
                attend(l, b, g)
            agather[l].send(b)

        gather = agather[l]
        weights[l][3].wait()
        gather.relay(0)
        for b in range(blocks):
            total = xg[l, tp, block_rows(b), :].astype(jnp.float32) + mixed_part(l, b, tp)
            for s in range(1, gather.n_x):
                total = total + mixed_part(l, b, gather.across(s, gather.core))
            if b + 1 < blocks:
                gather.relay(b + 1)
            for origin in gather.others():
                gather.wait_slot(b, origin)
                total = total + mixed_part(l, b, origin)
            result = total.astype(jnp.bfloat16)
            if l + 1 < layers:
                xg[l + 1, tp, block_rows(b), :] = result
                for c in range(b * per_block, (b + 1) * per_block):
                    xgather[l + 1].send(c)
            else:
                out[block_rows(b), :] = result

    for copy in gain_copies:
        copy.wait_send()
    for l in range(layers):
        for c in range(CHUNKS):
            xgather[l].finish(c, stream_piece(c) if l == 0 else None)
        for b in range(blocks):
            agather[l].finish(b)
            for g in range(groups):
                for t in range(2):
                    for ok, copy in direct_copies(l, t, g, b):
                        pl.when(ok)(copy.wait_send)
                    if relayed:
                        pl.when(odd_behind)(relay_copy(l, t, g, b).wait_send)


def per_device(n_tp, n_sp, stream, norm_gain, query_weight, key_weight, value_weight, out_weight, rel_bias):
    rows, width = stream.shape
    layers, full, head_cols = query_weight.shape
    heads_here = rel_bias.shape[1]
    head_dim = head_cols // heads_here
    groups = head_cols // LANES
    n_x = n_tp // 2
    shift = REACH // rows
    blocks = rows // PAIR
    any_space = pl.BlockSpec(memory_space=pl.ANY)
    vmem = pl.BlockSpec(memory_space=pltpu.VMEM)
    bf16, f32 = jnp.bfloat16, jnp.float32
    dma = pltpu.SemaphoreType.DMA
    return pl.pallas_call(
        functools.partial(kernel, n_tp, n_sp, head_dim),
        out_shape=jax.ShapeDtypeStruct((rows, width), bf16),
        in_specs=[any_space] * 7,
        out_specs=vmem,
        scratch_shapes=[
            pltpu.VMEM((layers, n_tp, rows, width), bf16),
            pltpu.VMEM((n_tp, layers, width), f32),
            pltpu.VMEM(rel_bias.shape, f32),
            pltpu.VMEM((layers, full, head_cols), bf16),
            pltpu.VMEM((layers, full, head_cols), bf16),
            pltpu.VMEM((layers, full, head_cols), bf16),
            pltpu.VMEM((layers, n_tp * head_cols, width), bf16),
            pltpu.VMEM((rows, full), bf16),
            pltpu.VMEM((layers, groups, (LANES // head_dim) * PAIR, BAND), f32),
            pltpu.VMEM((rows, head_cols), bf16),
            pltpu.VMEM((layers, groups, REACH + rows, LANES), bf16),
            pltpu.VMEM((layers, groups, REACH + rows, LANES), bf16),
            pltpu.VMEM((layers, n_tp, blocks, PAIR, head_cols), bf16),
            dma((layers, CHUNKS, 2 * n_x - 1)),
            dma((layers, CHUNKS, n_tp)),
            dma((layers, blocks, 2 * n_x - 1)),
            dma((layers, blocks, n_tp)),
            dma((layers, 2, groups * blocks, shift + 1)),
            dma((layers, 2, groups * blocks, shift)),
            dma((n_tp - 1,)),
            dma((n_tp - 1,)),
            dma((layers, 4)),
            dma((3,)),
        ],
        compiler_params=pltpu.CompilerParams(
            collective_id=0, has_side_effects=True, vmem_limit_bytes=60 * 1024 * 1024
        ),
    )(stream, norm_gain, query_weight, key_weight, value_weight, out_weight, rel_bias)


def solution(mesh):
    placed = (
        P("sp", "tp"),
        P(None, "tp"),
        P(None, None, "tp"),
        P(None, None, "tp"),
        P(None, None, "tp"),
        P(None, None, "tp"),
        P(None, "tp", None),
    )
    return jax.shard_map(
        functools.partial(per_device, mesh.shape["tp"], mesh.shape["sp"]),
        mesh=mesh, in_specs=placed, out_specs=P("sp", "tp"), check_vma=False,
    )
```
